32 devices in a mesh: grp: 2 (over y), ep: 8 (over z, x), tp: 2 (over core).
Axes of the slice: x: 2, y: 2, z: 4, core: 2. Of those that a mesh axis runs over, the one named last changes fastest.
Arguments:
- tokens: bfloat16 [384, 2048], P(('grp', 'ep')), parts along dimension 0, may hold values from -6 to 6
- norm_gain: float32 [2048], replicated, may hold values from 0.1 to 1.9
- routes: int32 [384, 4], P(('grp', 'ep')), parts along dimension 0, may hold values from 0 to 7, all different within a row; in each aligned block of 24 rows (0 to 23, 24 to 47, ...) at most 24 rows name the same one
- gate_scores: float32 [384, 4], P(('grp', 'ep')), parts along dimension 0, may hold values from 0.05 to 1
- w_gate: bfloat16 [8, 2048, 512], P('ep', None, 'tp'), may hold values from -1 to 1
- w_up: bfloat16 [8, 2048, 512], P('ep', None, 'tp'), may hold values from -1 to 1
- w_down: bfloat16 [8, 512, 2048], P('ep', 'tp'), may hold values from -0.0625 to 0.0625
Outputs:
- mixed: bfloat16 [384, 2048], P(('grp', 'ep')), parts along dimension 0
The draws below stay inside these ranges and needn't reach their ends.
There are 2 independent parts, one for each index of `grp`. The reference program is written for one: setup_inputs(seed, part) draws one part's arguments, and reference() takes and returns one part's arrays. A program takes and returns all parts, laid end to end along the dimension named above; an argument that names none is the same for every part. Nothing has to cross between parts.
Inputs may be any that keep to these rules, and one draw needn't show every extreme that they name: `routes`: each row names 4 different experts; among the 24 rows of one device no expert is named more than 24 times, a bound that some block reaches.
All inputs are finite; a program needn't handle non-finite values.
Results may differ from the reference program's by a relative error of at most 0.0077.
Values may be sent and summed in bfloat16 or wider, within the bound.
A program may use at most 64 MiB of HBM per device.

```python
import math
import jax
import jax.numpy as jnp
import numpy as np
from jax import lax

D = 2048
FF = 512
TOP_K = 4
TOK_DEV = 24
EXPERTS = 8
TOKENS = 192
CAP = 24
N_EP = 8
N_TP = 2


def levels(key, shape, cuts, smallest, largest):
    def one(axis_at, blocks):
        draws = jax.random.uniform(jax.random.fold_in(jax.random.fold_in(key, 6), axis_at), (blocks,), jnp.float32, smallest / len(cuts), largest / len(cuts))
        return jnp.repeat(jnp.exp(draws), shape[axis_at] // blocks).reshape((-1,) + (1,) * (len(shape) - axis_at - 1))

    loudness = one(*cuts[0])
    for cut in cuts[1:]:
        loudness = loudness * one(*cut)
    return loudness


def routed_block(rng, own, number, rows, number_of, top, reach, slope):
    sequence = jax.random.permutation(rng, number_of)
    crowded, ordinary = load_shares(number_of, rows * top, reach, slope, True), load_shares(number_of, rows * top, reach, slope, False)
    places = jnp.arange(number_of)

    def named(sizes, turn):
        used = int((sizes > 0).sum())
        fixed = max(1, used // 4)
        shifted = fixed + (places - fixed + turn * (used - fixed)) % max(1, number_of - fixed)
        return jnp.zeros((number_of,), jnp.int32).at[sequence[jnp.where(places < fixed, places, shifted)]].set(jnp.asarray(sizes, jnp.int32))

    sizes = jnp.where(number % 4 == 0, named(crowded, number // 4), named(ordinary, number - number // 4 - 1))
    mixed = jax.random.permutation(jax.random.fold_in(own, 3), number_of)
    giver, receiver = mixed[0:number_of // 2 * 2:2], mixed[1:number_of // 2 * 2:2]
    margin = jnp.minimum(sizes[giver] - 1, reach - sizes[receiver]) // 2
    margin = jnp.where((giver == sequence[0]) | (receiver == sequence[0]) | (sizes[receiver] == 0), 0, jnp.maximum(margin, 0))
    shifted = jax.random.randint(jax.random.fold_in(own, 4), (number_of // 2,), 0, 1 << 20) % (margin + 1)
    sizes = sizes.at[giver].add(-shifted).at[receiver].add(shifted)
    items = jnp.searchsorted(jnp.cumsum(sizes), jnp.arange(rows * top), side="right").astype(jnp.int32)
    table = items.reshape(top, rows).T
    table = table[jax.random.permutation(jax.random.fold_in(own, 1), rows)]
    turn = jax.random.randint(jax.random.fold_in(own, 2), (rows, 1), 0, top)
    return jnp.take_along_axis(table, (jnp.arange(top)[None, :] + turn) % top, axis=1)


def load_shares(number_of, total, reach, lean, full):
    weights = [(1 << 20) // math.isqrt(standing ** lean) + 1 for standing in range(1, number_of + 1)]
    largest = reach if full else min(reach, max(-(-total // number_of), total * weights[0] // sum(weights)))
    least = 1 if total - largest >= number_of - 1 else 0
    given, spare = [largest] + [least] * (number_of - 1), total - largest - least * (number_of - 1)
    while spare > 0:
        movable = [i for i in range(1, number_of) if given[i] < largest] or [i for i in range(1, number_of) if given[i] < reach]
        whole, budget = sum([weights[i] for i in movable]), spare
        for i in movable:
            addition = min(reach - given[i], max(1, budget * weights[i] // whole), spare)
            given[i] = given[i] + addition
            spare = spare - addition
    return np.array(given)


def bell_draw(own_key, dims, spread, reach, shards=(), held_as=jnp.bfloat16):
    entries = spread * jax.random.normal(own_key, dims, jnp.float32)
    if shards:
        entries = entries * levels(own_key, dims, shards, -0.22, 0.18)
    return jnp.clip(entries, -reach, reach).astype(held_as)


def setup_inputs(seed: int = 0, part: int = 0) -> dict:
    seeds = jax.random.split(jax.random.key(seed), 8)
    part_keys = jax.random.split(jax.random.fold_in(seeds[7], part), 8)
    tokens = bell_draw(part_keys[0], (TOKENS, D), 1.0, 6.0, ((0, 8),))
    norm_gain = jnp.clip(1.0 + 0.18 * jax.random.normal(seeds[1], (D,), jnp.float32), 0.1, 1.9)
    routes_keys = jax.random.split(jax.random.fold_in(part_keys[2], 1), TOKENS // TOK_DEV)
    routes_turns = jax.random.permutation(jax.random.fold_in(part_keys[2], 3), TOKENS // TOK_DEV)
    routes = jax.vmap(lambda own, number: routed_block(jax.random.fold_in(part_keys[2], 2), own, number, TOK_DEV, EXPERTS, TOP_K, CAP, 2))(routes_keys, routes_turns).reshape((TOKENS, TOP_K))
    gate_scores = jnp.clip(0.05 + 0.95 * jax.random.uniform(part_keys[3], (TOKENS, TOP_K), jnp.float32) ** levels(part_keys[3], (TOKENS, TOP_K), ((0, 8),), -0.2, 0.2), 0.05, 1.0)
    w_gate = bell_draw(seeds[4], (EXPERTS, D, FF), (3 * D ** -0.5), 1.0, ((0, 8), (2, 2)))
    w_up = bell_draw(seeds[5], (EXPERTS, D, FF), (3 * D ** -0.5), 1.0, ((0, 8), (2, 2)))
    w_down = bell_draw(seeds[6], (EXPERTS, FF, D), (16 * FF) ** -0.5, 0.0625, ((0, 8), (1, 2)))
    return {"tokens": tokens, "norm_gain": norm_gain, "routes": routes, "gate_scores": gate_scores, "w_gate": w_gate, "w_up": w_up, "w_down": w_down}


def clamped_unit(g, u):
    gate = jnp.minimum(g, 7.0)
    up = jnp.clip(u, -7.0, 7.0)
    return (up + 1.0) * gate * jax.nn.sigmoid(1.702 * gate)

def expert_apply(rows, wg, wu, wd):
    g = jnp.dot(rows, wg, preferred_element_type=jnp.float32)
    u = jnp.dot(rows, wu, preferred_element_type=jnp.float32)
    act = clamped_unit(g, u).astype(jnp.bfloat16)
    count = rows.shape[0]
    width = wd.shape[0]
    act_groups = act.reshape(count, N_TP, width // N_TP).astype(jnp.float32)
    down_groups = wd.reshape(N_TP, width // N_TP, wd.shape[1]).astype(jnp.float32)
    parts = jnp.einsum('rnf,nfd->nrd', act_groups, down_groups)
    parts = lax.optimization_barrier(parts.astype(jnp.bfloat16)).astype(jnp.float32)
    return lax.optimization_barrier(jnp.sum(parts, axis=0)).astype(jnp.bfloat16)

def reference(tokens, norm_gain, routes, gate_scores, w_gate, w_up, w_down):
    xf = tokens.astype(jnp.float32)
    normed = (xf * lax.rsqrt(lax.optimization_barrier(jnp.mean(xf * xf, axis=-1, keepdims=True)) + 1e-06) * norm_gain).astype(jnp.bfloat16)
    count = tokens.shape[0]
    width = tokens.shape[1]
    padded = jnp.concatenate([normed, jnp.zeros((1, width), jnp.bfloat16)], axis=0)
    slots = N_EP * CAP

    def one_expert(total, inputs):
        wg, wu, wd, expert = inputs
        chosen = routes == expert
        hit = jnp.any(chosen, axis=1)
        weight = lax.optimization_barrier(jnp.sum(jnp.where(chosen, gate_scores, 0.0), axis=1))
        weight = jnp.concatenate([weight, jnp.zeros((1,), jnp.float32)])
        index = jnp.nonzero(hit, size=slots, fill_value=count)[0].astype(jnp.int32)
        outputs = expert_apply(padded[index], wg, wu, wd)
        contrib = weight[index][:, None] * outputs.astype(jnp.float32)
        return (total.at[index].add(contrib), None)
    start = jnp.zeros((count + 1, width), jnp.float32)
    experts = jnp.arange(w_gate.shape[0], dtype=jnp.int32)
    total, _ = lax.scan(one_expert, start, (w_gate, w_up, w_down, experts))
    return total[:count].astype(jnp.bfloat16)
```

```python
import functools

import jax
import jax.numpy as jnp
from jax import lax
from jax.experimental import pallas as pl
from jax.experimental.pallas import tpu as pltpu
from jax.sharding import PartitionSpec as P

MESH = pl.DeviceIdType.MESH
LANES = 128


def clamped_unit(g, u):
    gate = jnp.minimum(g, 7.0)
    up = jnp.clip(u, -7.0, 7.0)
    return (up + 1.0) * gate * jax.nn.sigmoid(1.702 * gate)


def expert_rows(rows, wg, wu, wd):
    g = jnp.dot(rows, wg, preferred_element_type=jnp.float32)
    u = jnp.dot(rows, wu, preferred_element_type=jnp.float32)
    act = clamped_unit(g, u).astype(jnp.bfloat16)
    part = jnp.dot(act, wd, preferred_element_type=jnp.float32)
    part = lax.optimization_barrier(part.astype(jnp.bfloat16)).astype(jnp.float32)
    total = lax.psum(part.astype(jnp.bfloat16), "tp")
    return total


def finish(mixed):
    result = mixed.astype(jnp.bfloat16)
    return result


def slot_table(routes, scores, experts, capacity):
    count = routes.shape[0]
    chosen = routes[:, :, None] == experts[None, None, :]
    hit = jnp.any(chosen, axis=1).astype(jnp.int32)
    weight = jnp.sum(jnp.where(chosen, scores[:, :, None], 0.0), axis=1)
    rank = jnp.cumsum(hit, axis=0) - hit
    places = jnp.arange(capacity, dtype=jnp.int32)
    match = (hit[:, :, None] == 1) & (rank[:, :, None] == places[None, None, :])
    row_ids = jnp.arange(count, dtype=jnp.int32)[:, None, None]
    filled = jnp.any(match, axis=0)
    slot_tok = jnp.sum(jnp.where(match, row_ids, 0), axis=0) + count * (
        1 - filled.astype(jnp.int32)
    )
    slot_w = jnp.sum(jnp.where(match, weight[:, :, None], 0.0), axis=0)
    return (slot_tok, slot_w)


def exchange_body(tokens, norm_gain, routes, gate_scores, w_gate, w_up, w_down):
    count, width = tokens.shape
    top = routes.shape[1]
    nexp = lax.axis_size("ep")
    capacity = max(2, min(count, 2 * count * top // nexp))
    wg, wu, wd = (w_gate[0], w_up[0], w_down[0])
    xf = tokens.astype(jnp.float32)
    normed = (xf * lax.rsqrt(jnp.mean(xf * xf, axis=-1, keepdims=True) + 1e-06) * norm_gain).astype(
        jnp.bfloat16
    )
    experts = jnp.arange(nexp, dtype=jnp.int32)
    slot_tok, slot_w = slot_table(routes, gate_scores, experts, capacity)
    padded = jnp.concatenate([normed, jnp.zeros((1, width), jnp.bfloat16)], axis=0)
    outgoing = padded[slot_tok]
    received = lax.all_to_all(outgoing, "ep", split_axis=0, concat_axis=0, tiled=True)
    sources, places, _ = received.shape
    outputs = expert_rows(received.reshape(sources * places, width), wg, wu, wd)
    returned = lax.all_to_all(
        outputs.reshape(sources, places, outputs.shape[1]),
        "ep",
        split_axis=0,
        concat_axis=0,
        tiled=True,
    )
    flat_tok = slot_tok.reshape(-1)
    token_ids = jnp.arange(count, dtype=jnp.int32)
    combine = jnp.where(flat_tok[None, :] == token_ids[:, None], slot_w.reshape(-1)[None, :], 0.0)
    mixed = jnp.dot(
        combine,
        returned.reshape(-1, returned.shape[2]).astype(jnp.float32),
        precision=lax.Precision.HIGHEST,
    )
    return finish(mixed)


def moe_kernel(
    nz,
    tok_ref, gain_ref, routes_ref, score_ref, wg_hbm, wu_hbm, wd_hbm,
    out_ref,
    gath, wg, wu, wd, contrib, from_x, summed, from_z, res,
    w_loc, w_send, w_recv, z_send, z_recv, x_send, x_recv,
    rx_send, rx_recv, rz_send, rz_recv, f_send, f_recv,
):
    ep, tp = lax.axis_index("ep"), lax.axis_index("tp")
    z, x = ep // 2, ep % 2
    home = x == tp
    count, width = tok_ref.shape

    def at_z(zz):
        return {"ep": zz * 2 + x, "tp": tp}

    x_peer = {"ep": z * 2 + 1 - x, "tp": tp}
    sibling = {"ep": ep, "tp": 1 - tp}
    others = [(z + k) % nz for k in range(1, nz)]

    barrier = pltpu.get_barrier_semaphore()
    for zz in others:
        pl.semaphore_signal(barrier, inc=1, device_id=at_z(zz), device_id_type=MESH)
    pl.semaphore_signal(barrier, inc=1, device_id=x_peer, device_id_type=MESH)
    pl.semaphore_signal(barrier, inc=1, device_id=sibling, device_id_type=MESH)

    weights = ((wg_hbm, wg), (wu_hbm, wu), (wd_hbm, wd))
    local = [
        pltpu.make_async_copy(src.at[0], dst.at[tp], w_loc.at[i])
        for i, (src, dst) in enumerate(weights)
    ]
    shared = [
        pltpu.make_async_remote_copy(
            src.at[0], dst.at[tp], w_send.at[i], w_recv.at[i], device_id=sibling, device_id_type=MESH
        )
        for i, (src, dst) in enumerate(weights)
    ]
    for c in local:
        c.start()

    @pl.when(home)
    def _():
        xf = tok_ref[...].astype(jnp.float32)
        scale = lax.rsqrt(jnp.mean(xf * xf, axis=-1, keepdims=True) + 1e-06)
        gath[z, :, :width] = (xf * scale * gain_ref[...]).astype(jnp.bfloat16)
        lane = lax.broadcasted_iota(jnp.int32, (count, LANES), 1)
        half = LANES // 2
        expert = lane % half
        w = jnp.zeros((count, LANES), jnp.float32)
        for k in range(routes_ref.shape[1]):
            w = w + jnp.where(routes_ref[:, k : k + 1] == expert, score_ref[:, k : k + 1], 0.0)
        high = w.astype(jnp.bfloat16)
        low = (w - high.astype(jnp.float32)).astype(jnp.bfloat16)
        gath[z, :, width:] = jnp.where(
            lane < half, high.astype(jnp.float32), low.astype(jnp.float32)
        ).astype(jnp.bfloat16)

    pl.semaphore_wait(barrier, nz + 1)
    for c in shared:
        c.start()

    def along_z(zz, slot):
        return pltpu.make_async_remote_copy(
            gath.at[slot], gath.at[slot], z_send.at[zz], z_recv.at[slot],
            device_id=at_z(zz), device_id_type=MESH,
        )

    def across_x(slot):
        return pltpu.make_async_remote_copy(
            gath.at[slot], gath.at[slot], x_send.at[slot], x_recv.at[slot],
            device_id=x_peer, device_id_type=MESH,
        )

    order = [z] + [(z + k) % nz for k in ORDER if k < nz]

    @pl.when(home)
    def _():
        for zz in order[1:]:
            along_z(zz, z).start()
        across_x(z).start()

    def arrive(slot, own):
        @pl.when(home)
        def _():
            if not own:
                along_z(slot, slot).wait_recv()
                across_x(slot).start()

        @pl.when(jnp.logical_not(home))
        def _():
            across_x(slot).wait_recv()

    def compute(slots):
        rows = jnp.concatenate(
            [gath[s, :, :width].astype(jnp.float32) for s in slots], axis=0
        ).astype(jnp.bfloat16)
        acts = []
        for j in range(2):
            g = jnp.dot(rows, wg[j], preferred_element_type=jnp.float32)
            u = jnp.dot(rows, wu[j], preferred_element_type=jnp.float32)
            gate = jnp.minimum(g, 7.0)
            up = jnp.clip(u, -7.0, 7.0)
            acts.append(((up + 1.0) * gate * jax.nn.sigmoid(1.702 * gate)).astype(jnp.bfloat16))
        lane = lax.broadcasted_iota(jnp.int32, (count, LANES), 1)
        mine = lane % (LANES // 2) == ep
        weight = [
            jnp.sum(
                jnp.where(mine, gath[s, :, width:].astype(jnp.float32), 0.0), axis=1, keepdims=True
            )
            for s in slots
        ]
        step = width // 4
        for c in range(0, width, step):
            y = jnp.dot(acts[0], wd[0, :, c : c + step], preferred_element_type=jnp.float32)
            y = y + jnp.dot(acts[1], wd[1, :, c : c + step], preferred_element_type=jnp.float32)
            for i, s in enumerate(slots):
                contrib[s, :, c : c + step] = (
                    y[i * count : (i + 1) * count] * weight[i]
                ).astype(jnp.bfloat16)

    def back_x(slot):
        return pltpu.make_async_remote_copy(
            contrib.at[slot], from_x.at[slot], rx_send.at[slot], rx_recv.at[slot],
            device_id=x_peer, device_id_type=MESH,
        )

    def back_z(zz, slot):
        return pltpu.make_async_remote_copy(
            summed.at[zz], from_z.at[slot], rz_send.at[zz], rz_recv.at[slot],
            device_id=at_z(zz), device_id_type=MESH,
        )

    for i, slot in enumerate(order):
        arrive(slot, i == 0)
    for c in local:
        c.wait()
    for c in shared:
        c.wait()
    compute(order)

    back = order[1:] + order[:1]

    @pl.when(jnp.logical_not(home))
    def _():
        for slot in back:
            back_x(slot).start()

    final = pltpu.make_async_remote_copy(
        res, res, f_send, f_recv, device_id=sibling, device_id_type=MESH
    )

    @pl.when(home)
    def _():
        for slot in back[:-1]:
            back_x(slot).wait_recv()
            summed[slot] = (
                contrib[slot].astype(jnp.float32) + from_x[slot].astype(jnp.float32)
            ).astype(jnp.bfloat16)
            back_z(slot, z).start()
        back_x(z).wait_recv()
        total = contrib[z].astype(jnp.float32) + from_x[z].astype(jnp.float32)
        for slot in back[:-1]:
            back_z(slot, slot).wait_recv()
            total = total + from_z[slot].astype(jnp.float32)
        res[...] = total.astype(jnp.bfloat16)
        final.start()
        out_ref[...] = total.astype(out_ref.dtype)
        for zz in order[1:]:
            along_z(zz, z).wait_send()
            back_z(zz, z).wait_send()
        for slot in order:
            across_x(slot).wait_send()
        final.wait_send()

    @pl.when(jnp.logical_not(home))
    def _():
        for slot in order:
            back_x(slot).wait_send()
        final.wait_recv()
        out_ref[...] = res[...].astype(out_ref.dtype)


ORDER = (1, 3, 2)


def gather_body(tokens, norm_gain, routes, gate_scores, w_gate, w_up, w_down):
    count, width = tokens.shape
    nz = lax.axis_size("ep") // 2
    hidden = w_gate.shape[2]
    bf16 = jnp.bfloat16
    dma = pltpu.SemaphoreType.DMA
    block = (nz, count, width)
    vmem = pl.BlockSpec(memory_space=pltpu.VMEM)
    hbm = pl.BlockSpec(memory_space=pl.ANY)
    out = pl.pallas_call(
        functools.partial(moe_kernel, nz),
        out_shape=jax.ShapeDtypeStruct((count, width), bf16),
        in_specs=[vmem] * 4 + [hbm] * 3,
        out_specs=vmem,
        scratch_shapes=[
            pltpu.VMEM((nz, count, width + LANES), bf16),
            pltpu.VMEM((2, width, hidden), bf16),
            pltpu.VMEM((2, width, hidden), bf16),
            pltpu.VMEM((2, hidden, width), bf16),
            pltpu.VMEM(block, bf16),
            pltpu.VMEM(block, bf16),
            pltpu.VMEM(block, bf16),
            pltpu.VMEM(block, bf16),
            pltpu.VMEM((count, width), bf16),
        ]
        + [dma((3,))] * 3
        + [dma((nz,))] * 8
        + [dma(()), dma(())],
        compiler_params=pltpu.CompilerParams(collective_id=0, has_side_effects=True),
        name="moe",
    )(tokens, norm_gain.reshape(1, width), routes, gate_scores, w_gate, w_up, w_down)
    return out


def body(tokens, norm_gain, routes, gate_scores, w_gate, w_up, w_down):
    nexp = lax.axis_size("ep")
    every_row = 2 * routes.shape[1] >= nexp
    pairs = lax.axis_size("tp") == 2 and nexp % 2 == 0
    one = exchange_body
    if every_row and pairs and w_gate.shape[0] == 1 and 2 * nexp <= LANES:
        one = gather_body
    return one(tokens, norm_gain, routes, gate_scores, w_gate, w_up, w_down)


def solution(mesh):
    in_specs = (
        P(("grp", "ep"), None),
        P(),
        P(("grp", "ep"), None),
        P(("grp", "ep"), None),
        P("ep", None, "tp"),
        P("ep", None, "tp"),
        P("ep", "tp", None),
    )
    out_specs = P(("grp", "ep"), None)
    return jax.shard_map(body, mesh=mesh, in_specs=in_specs, out_specs=out_specs, check_vma=False)
```

```python
import functools

import jax
import jax.numpy as jnp
from jax import lax
from jax.experimental import pallas as pl
from jax.experimental.pallas import tpu as pltpu
from jax.sharding import PartitionSpec as P

MESH = pl.DeviceIdType.MESH
LANES = 128


def clamped_unit(g, u):
    gate = jnp.minimum(g, 7.0)
    up = jnp.clip(u, -7.0, 7.0)
    return (up + 1.0) * gate * jax.nn.sigmoid(1.702 * gate)


def expert_rows(rows, wg, wu, wd):
    g = jnp.dot(rows, wg, preferred_element_type=jnp.float32)
    u = jnp.dot(rows, wu, preferred_element_type=jnp.float32)
    act = clamped_unit(g, u).astype(jnp.bfloat16)
    part = jnp.dot(act, wd, preferred_element_type=jnp.float32)
    part = lax.optimization_barrier(part.astype(jnp.bfloat16)).astype(jnp.float32)
    total = lax.psum(part.astype(jnp.bfloat16), "tp")
    return total


def finish(mixed):
    result = mixed.astype(jnp.bfloat16)
    return result


def slot_table(routes, scores, experts, capacity):
    count = routes.shape[0]
    chosen = routes[:, :, None] == experts[None, None, :]
    hit = jnp.any(chosen, axis=1).astype(jnp.int32)
    weight = jnp.sum(jnp.where(chosen, scores[:, :, None], 0.0), axis=1)
    rank = jnp.cumsum(hit, axis=0) - hit
    places = jnp.arange(capacity, dtype=jnp.int32)
    match = (hit[:, :, None] == 1) & (rank[:, :, None] == places[None, None, :])
    row_ids = jnp.arange(count, dtype=jnp.int32)[:, None, None]
    filled = jnp.any(match, axis=0)
    slot_tok = jnp.sum(jnp.where(match, row_ids, 0), axis=0) + count * (
        1 - filled.astype(jnp.int32)
    )
    slot_w = jnp.sum(jnp.where(match, weight[:, :, None], 0.0), axis=0)
    return (slot_tok, slot_w)


def exchange_body(tokens, norm_gain, routes, gate_scores, w_gate, w_up, w_down):
    count, width = tokens.shape
    top = routes.shape[1]
    nexp = lax.axis_size("ep")
    capacity = max(2, min(count, 2 * count * top // nexp))
    wg, wu, wd = (w_gate[0], w_up[0], w_down[0])
    xf = tokens.astype(jnp.float32)
    normed = (xf * lax.rsqrt(jnp.mean(xf * xf, axis=-1, keepdims=True) + 1e-06) * norm_gain).astype(
        jnp.bfloat16
    )
    experts = jnp.arange(nexp, dtype=jnp.int32)
    slot_tok, slot_w = slot_table(routes, gate_scores, experts, capacity)
    padded = jnp.concatenate([normed, jnp.zeros((1, width), jnp.bfloat16)], axis=0)
    outgoing = padded[slot_tok]
    received = lax.all_to_all(outgoing, "ep", split_axis=0, concat_axis=0, tiled=True)
    sources, places, _ = received.shape
    outputs = expert_rows(received.reshape(sources * places, width), wg, wu, wd)
    returned = lax.all_to_all(
        outputs.reshape(sources, places, outputs.shape[1]),
        "ep",
        split_axis=0,
        concat_axis=0,
        tiled=True,
    )
    flat_tok = slot_tok.reshape(-1)
    token_ids = jnp.arange(count, dtype=jnp.int32)
    combine = jnp.where(flat_tok[None, :] == token_ids[:, None], slot_w.reshape(-1)[None, :], 0.0)
    mixed = jnp.dot(
        combine,
        returned.reshape(-1, returned.shape[2]).astype(jnp.float32),
        precision=lax.Precision.HIGHEST,
    )
    return finish(mixed)


def moe_kernel(
    nz,
    tok_hbm, gain_hbm, routes_hbm, score_hbm, wg_hbm, wu_hbm, wd_hbm,
    out_ref,
    tok_ref, gain_ref, routes_ref, score_ref, gath, wg, wu, wd, contrib, from_x, summed, from_z, res,
    in_sem, w_loc, w_send, w_recv, z_send, z_recv, x_send, x_recv,
    rx_send, rx_recv, rz_send, rz_recv, f_send, f_recv,
):
    ep, tp = lax.axis_index("ep"), lax.axis_index("tp")
    z, x = ep // 2, ep % 2
    home = x == tp
    count, width = tok_hbm.shape

    def at_z(zz):
        return {"ep": zz * 2 + x, "tp": tp}

    x_peer = {"ep": z * 2 + 1 - x, "tp": tp}
    sibling = {"ep": ep, "tp": 1 - tp}
    others = [(z + k) % nz for k in range(1, nz)]

    barrier = pltpu.get_barrier_semaphore()
    for zz in others:
        pl.semaphore_signal(barrier, inc=1, device_id=at_z(zz), device_id_type=MESH)
    pl.semaphore_signal(barrier, inc=1, device_id=x_peer, device_id_type=MESH)
    pl.semaphore_signal(barrier, inc=1, device_id=sibling, device_id_type=MESH)

    weights = ((wg_hbm, wg), (wu_hbm, wu), (wd_hbm, wd))
    local = [
        pltpu.make_async_copy(src.at[0], dst.at[tp], w_loc.at[i])
        for i, (src, dst) in enumerate(weights)
    ]
    shared = [
        pltpu.make_async_remote_copy(
            src.at[0], dst.at[tp], w_send.at[i], w_recv.at[i], device_id=sibling, device_id_type=MESH
        )
        for i, (src, dst) in enumerate(weights)
    ]
    inputs = [
        pltpu.make_async_copy(src, dst, in_sem.at[i])
        for i, (src, dst) in enumerate(
            ((tok_hbm, tok_ref), (gain_hbm, gain_ref), (routes_hbm, routes_ref), (score_hbm, score_ref))
        )
    ]
    for c in inputs + local:
        c.start()
    for c in inputs:
        c.wait()

    @pl.when(home)
    def _():
        xf = tok_ref[...].astype(jnp.float32)
        scale = lax.rsqrt(jnp.mean(xf * xf, axis=-1, keepdims=True) + 1e-06)
        gath[z, :, :width] = (xf * scale * gain_ref[...]).astype(jnp.bfloat16)
        line = lax.broadcasted_iota(jnp.int32, (LANES, count), 0)
        half = LANES // 2
        expert = line % half
        w = jnp.zeros((LANES, count), jnp.float32)
        for k in range(routes_ref.shape[0]):
            w = w + jnp.where(routes_ref[k : k + 1, :] == expert, score_ref[k : k + 1, :], 0.0)
        high = w.astype(jnp.bfloat16).astype(jnp.float32)
        gath[z, :, width:] = jnp.where(line < half, high, w - high).T.astype(jnp.bfloat16)

    pl.semaphore_wait(barrier, nz + 1)
    for c in shared:
        c.start()

    def along_z(zz, slot):
        return pltpu.make_async_remote_copy(
            gath.at[slot], gath.at[slot], z_send.at[zz], z_recv.at[slot],
            device_id=at_z(zz), device_id_type=MESH,
        )

    def across_x(slot):
        return pltpu.make_async_remote_copy(
            gath.at[slot], gath.at[slot], x_send.at[slot], x_recv.at[slot],
            device_id=x_peer, device_id_type=MESH,
        )

    order = [z] + [(z + k) % nz for k in ORDER if k < nz]

    @pl.when(home)
    def _():
        for zz in order[1:]:
            along_z(zz, z).start()
        across_x(z).start()

    def arrive(slot, own):
        @pl.when(home)
        def _():
            if not own:
                along_z(slot, slot).wait_recv()
                across_x(slot).start()

        @pl.when(jnp.logical_not(home))
        def _():
            across_x(slot).wait_recv()

    def compute(slots):
        rows = jnp.concatenate(
            [gath[s, :, :width].astype(jnp.float32) for s in slots], axis=0
        ).astype(jnp.bfloat16)
        acts = []
        for j in range(2):
            g = jnp.dot(rows, wg[j], preferred_element_type=jnp.float32)
            u = jnp.dot(rows, wu[j], preferred_element_type=jnp.float32)
            gate = jnp.minimum(g, 7.0)
            up = jnp.clip(u, -7.0, 7.0)
            acts.append(((up + 1.0) * gate * jax.nn.sigmoid(1.702 * gate)).astype(jnp.bfloat16))
        lane = lax.broadcasted_iota(jnp.int32, (count, LANES), 1)
        mine = lane % (LANES // 2) == ep
        weight = [
            jnp.sum(
                jnp.where(mine, gath[s, :, width:].astype(jnp.float32), 0.0), axis=1, keepdims=True
            )
            for s in slots
        ]
        step = width // 4
        for c in range(0, width, step):
            y = jnp.dot(acts[0], wd[0, :, c : c + step], preferred_element_type=jnp.float32)
            y = y + jnp.dot(acts[1], wd[1, :, c : c + step], preferred_element_type=jnp.float32)
            for i, s in enumerate(slots):
                contrib[s, :, c : c + step] = (
                    y[i * count : (i + 1) * count] * weight[i]
                ).astype(jnp.bfloat16)

    def back_x(slot):
        return pltpu.make_async_remote_copy(
            contrib.at[slot], from_x.at[slot], rx_send.at[slot], rx_recv.at[slot],
            device_id=x_peer, device_id_type=MESH,
        )

    def back_z(zz, slot):
        return pltpu.make_async_remote_copy(
            summed.at[zz], from_z.at[slot], rz_send.at[zz], rz_recv.at[slot],
            device_id=at_z(zz), device_id_type=MESH,
        )

    for i, slot in enumerate(order):
        arrive(slot, i == 0)
    for c in local:
        c.wait()
    for c in shared:
        c.wait()
    compute(order)

    back = order[1:] + order[:1]

    @pl.when(jnp.logical_not(home))
    def _():
        for slot in back:
            back_x(slot).start()

    final = pltpu.make_async_remote_copy(
        res, res, f_send, f_recv, device_id=sibling, device_id_type=MESH
    )

    @pl.when(home)
    def _():
        for slot in back[:-1]:
            back_x(slot).wait_recv()
            summed[slot] = (
                contrib[slot].astype(jnp.float32) + from_x[slot].astype(jnp.float32)
            ).astype(jnp.bfloat16)
            back_z(slot, z).start()
        back_x(z).wait_recv()
        total = contrib[z].astype(jnp.float32) + from_x[z].astype(jnp.float32)
        for slot in back[:-1]:
            back_z(slot, slot).wait_recv()
            total = total + from_z[slot].astype(jnp.float32)
        res[...] = total.astype(jnp.bfloat16)
        final.start()
        out_ref[...] = total.astype(out_ref.dtype)
        for zz in order[1:]:
            along_z(zz, z).wait_send()
            back_z(zz, z).wait_send()
        for slot in order:
            across_x(slot).wait_send()
        final.wait_send()

    @pl.when(jnp.logical_not(home))
    def _():
        for slot in order:
            back_x(slot).wait_send()
        final.wait_recv()
        out_ref[...] = res[...].astype(out_ref.dtype)


ORDER = (1, 3, 2)
VMEM_BYTES = 67043328


def gather_body(tokens, norm_gain, routes, gate_scores, w_gate, w_up, w_down):
    count, width = tokens.shape
    top = routes.shape[1]
    nz = lax.axis_size("ep") // 2
    hidden = w_gate.shape[2]
    bf16 = jnp.bfloat16
    dma = pltpu.SemaphoreType.DMA
    block = (nz, count, width)
    vmem = pl.BlockSpec(memory_space=pltpu.VMEM)
    hbm = pl.BlockSpec(memory_space=pltpu.HBM)
    out = pl.pallas_call(
        functools.partial(moe_kernel, nz),
        out_shape=jax.ShapeDtypeStruct((count, width), bf16),
        in_specs=[hbm] * 7,
        out_specs=vmem,
        scratch_shapes=[
            pltpu.VMEM((count, width), bf16),
            pltpu.VMEM((1, width), jnp.float32),
            pltpu.VMEM((top, count), jnp.int32),
            pltpu.VMEM((top, count), jnp.float32),
            pltpu.VMEM((nz, count, width + LANES), bf16),
            pltpu.VMEM((2, width, hidden), bf16),
            pltpu.VMEM((2, width, hidden), bf16),
            pltpu.VMEM((2, hidden, width), bf16),
            pltpu.VMEM(block, bf16),
            pltpu.VMEM(block, bf16),
            pltpu.VMEM(block, bf16),
            pltpu.VMEM(block, bf16),
            pltpu.VMEM((count, width), bf16),
        ]
        + [dma((4,))]
        + [dma((3,))] * 3
        + [dma((nz,))] * 8
        + [dma(()), dma(())],
        compiler_params=pltpu.CompilerParams(
            collective_id=0, has_side_effects=True, vmem_limit_bytes=VMEM_BYTES
        ),
        name="moe",
    )(tokens, norm_gain.reshape(1, width), routes.T, gate_scores.T, w_gate, w_up, w_down)
    return out


def body(tokens, norm_gain, routes, gate_scores, w_gate, w_up, w_down):
    nexp = lax.axis_size("ep")
    every_row = 2 * routes.shape[1] >= nexp
    pairs = lax.axis_size("tp") == 2 and nexp % 2 == 0
    one = exchange_body
    if every_row and pairs and w_gate.shape[0] == 1 and 2 * nexp <= LANES:
        one = gather_body
    return one(tokens, norm_gain, routes, gate_scores, w_gate, w_up, w_down)


def solution(mesh):
    in_specs = (
        P(("grp", "ep"), None),
        P(),
        P(("grp", "ep"), None),
        P(("grp", "ep"), None),
        P("ep", None, "tp"),
        P("ep", None, "tp"),
        P("ep", "tp", None),
    )
    out_specs = P(("grp", "ep"), None)
    return jax.shard_map(body, mesh=mesh, in_specs=in_specs, out_specs=out_specs, check_vma=False)
```

```python
import functools

import jax
import jax.numpy as jnp
from jax import lax
from jax.experimental import pallas as pl
from jax.experimental.pallas import tpu as pltpu
from jax.sharding import PartitionSpec as P

MESH = pl.DeviceIdType.MESH
LANES = 128


def clamped_unit(g, u):
    gate = jnp.minimum(g, 7.0)
    up = jnp.clip(u, -7.0, 7.0)
    return (up + 1.0) * gate * jax.nn.sigmoid(1.702 * gate)


def expert_rows(rows, wg, wu, wd):
    g = jnp.dot(rows, wg, preferred_element_type=jnp.float32)
    u = jnp.dot(rows, wu, preferred_element_type=jnp.float32)
    act = clamped_unit(g, u).astype(jnp.bfloat16)
    part = jnp.dot(act, wd, preferred_element_type=jnp.float32)
    part = lax.optimization_barrier(part.astype(jnp.bfloat16)).astype(jnp.float32)
    total = lax.psum(part.astype(jnp.bfloat16), "tp")
    return total


def finish(mixed):
    result = mixed.astype(jnp.bfloat16)
    return result


def slot_table(routes, scores, experts, capacity):
    count = routes.shape[0]
    chosen = routes[:, :, None] == experts[None, None, :]
    hit = jnp.any(chosen, axis=1).astype(jnp.int32)
    weight = jnp.sum(jnp.where(chosen, scores[:, :, None], 0.0), axis=1)
    rank = jnp.cumsum(hit, axis=0) - hit
    places = jnp.arange(capacity, dtype=jnp.int32)
    match = (hit[:, :, None] == 1) & (rank[:, :, None] == places[None, None, :])
    row_ids = jnp.arange(count, dtype=jnp.int32)[:, None, None]
    filled = jnp.any(match, axis=0)
    slot_tok = jnp.sum(jnp.where(match, row_ids, 0), axis=0) + count * (
        1 - filled.astype(jnp.int32)
    )
    slot_w = jnp.sum(jnp.where(match, weight[:, :, None], 0.0), axis=0)
    return (slot_tok, slot_w)


def exchange_body(tokens, norm_gain, routes, gate_scores, w_gate, w_up, w_down):
    count, width = tokens.shape
    top = routes.shape[1]
    nexp = lax.axis_size("ep")
    capacity = max(2, min(count, 2 * count * top // nexp))
    wg, wu, wd = (w_gate[0], w_up[0], w_down[0])
    xf = tokens.astype(jnp.float32)
    normed = (xf * lax.rsqrt(jnp.mean(xf * xf, axis=-1, keepdims=True) + 1e-06) * norm_gain).astype(
        jnp.bfloat16
    )
    experts = jnp.arange(nexp, dtype=jnp.int32)
    slot_tok, slot_w = slot_table(routes, gate_scores, experts, capacity)
    padded = jnp.concatenate([normed, jnp.zeros((1, width), jnp.bfloat16)], axis=0)
    outgoing = padded[slot_tok]
    received = lax.all_to_all(outgoing, "ep", split_axis=0, concat_axis=0, tiled=True)
    sources, places, _ = received.shape
    outputs = expert_rows(received.reshape(sources * places, width), wg, wu, wd)
    returned = lax.all_to_all(
        outputs.reshape(sources, places, outputs.shape[1]),
        "ep",
        split_axis=0,
        concat_axis=0,
        tiled=True,
    )
    flat_tok = slot_tok.reshape(-1)
    token_ids = jnp.arange(count, dtype=jnp.int32)
    combine = jnp.where(flat_tok[None, :] == token_ids[:, None], slot_w.reshape(-1)[None, :], 0.0)
    mixed = jnp.dot(
        combine,
        returned.reshape(-1, returned.shape[2]).astype(jnp.float32),
        precision=lax.Precision.HIGHEST,
    )
    return finish(mixed)


VMEM_BYTES = 66500000
ROWS = 8


def moe_kernel(
    nz,
    tok_hbm, gain_hbm, routes_hbm, score_hbm, wg_hbm, wu_hbm, wd_hbm,
    out_ref,
    tok_ref, gain_ref, routes_ref, score_ref, gath, wg, wu, wd, contrib, from_x, summed, from_z, res,
    in_sem, w_loc, w_send, w_recv, z_send, z_recv, x_send, x_recv,
    rx_send, rx_recv, rz_send, rz_recv, f_send, f_recv,
):
    ep, tp = lax.axis_index("ep"), lax.axis_index("tp")
    z, x = ep // 2, ep % 2
    home = x == tp
    count, width = tok_hbm.shape

    def at_z(zz):
        return {"ep": zz * 2 + x, "tp": tp}

    x_peer = {"ep": z * 2 + 1 - x, "tp": tp}
    sibling = {"ep": ep, "tp": 1 - tp}
    low = (z < nz // 2).astype(jnp.int32)

    def far_first(k):
        down = nz - 1 - k
        down = down - (down <= z).astype(jnp.int32)
        up = k + (k >= z).astype(jnp.int32)
        return low * down + (1 - low) * up

    others = [far_first(k) for k in range(nz - 1)]
    order = [z] + others[::-1]
    pieces = [pl.ds(r, ROWS) for r in range(0, count, ROWS)]

    barrier = pltpu.get_barrier_semaphore()
    for zz in others:
        pl.semaphore_signal(barrier, inc=1, device_id=at_z(zz), device_id_type=MESH)
    pl.semaphore_signal(barrier, inc=1, device_id=x_peer, device_id_type=MESH)
    pl.semaphore_signal(barrier, inc=1, device_id=sibling, device_id_type=MESH)

    weights = ((wg_hbm, wg), (wu_hbm, wu), (wd_hbm, wd))
    local = [
        pltpu.make_async_copy(src.at[0], dst.at[tp], w_loc.at[i])
        for i, (src, dst) in enumerate(weights)
    ]
    shared = [
        pltpu.make_async_remote_copy(
            src.at[0], dst.at[tp], w_send.at[i], w_recv.at[i], device_id=sibling, device_id_type=MESH
        )
        for i, (src, dst) in enumerate(weights)
    ]
    inputs = [
        pltpu.make_async_copy(src, dst, in_sem.at[i])
        for i, (src, dst) in enumerate(
            ((tok_hbm, tok_ref), (gain_hbm, gain_ref), (routes_hbm, routes_ref), (score_hbm, score_ref))
        )
    ]
    for c in local:
        c.start()

    @pl.when(home)
    def _():
        for c in inputs:
            c.start()
        for c in inputs:
            c.wait()
        xf = tok_ref[...].astype(jnp.float32)
        scale = lax.rsqrt(jnp.mean(xf * xf, axis=-1, keepdims=True) + 1e-06)
        gath[z, :, :width] = (xf * scale * gain_ref[...]).astype(jnp.bfloat16)
        line = lax.broadcasted_iota(jnp.int32, (LANES, count), 0)
        half = LANES // 2
        expert = line % half
        w = jnp.zeros((LANES, count), jnp.float32)
        for k in range(routes_ref.shape[0]):
            w = w + jnp.where(routes_ref[k : k + 1, :] == expert, score_ref[k : k + 1, :], 0.0)
        high = w.astype(jnp.bfloat16).astype(jnp.float32)
        gath[z, :, width:] = jnp.where(line < half, high, w - high).T.astype(jnp.bfloat16)

    pl.semaphore_wait(barrier, nz + 1)
    for c in shared:
        c.start()

    def along_z(zz, slot, c):
        part = gath.at[slot, pieces[c]]
        return pltpu.make_async_remote_copy(
            part, part, z_send.at[zz, c], z_recv.at[slot, c],
            device_id=at_z(zz), device_id_type=MESH,
        )

    def across_x(slot, c):
        part = gath.at[slot, pieces[c]]
        return pltpu.make_async_remote_copy(
            part, part, x_send.at[slot, c], x_recv.at[slot, c],
            device_id=x_peer, device_id_type=MESH,
        )

    def compute(slots):
        rows = jnp.concatenate(
            [gath[s, :, :width].astype(jnp.float32) for s in slots], axis=0
        ).astype(jnp.bfloat16)
        acts = []
        for j in range(2):
            g = jnp.dot(rows, wg[j], preferred_element_type=jnp.float32)
            u = jnp.dot(rows, wu[j], preferred_element_type=jnp.float32)
            gate = jnp.minimum(g, 7.0)
            up = jnp.clip(u, -7.0, 7.0)
            acts.append(((up + 1.0) * gate * jax.nn.sigmoid(1.702 * gate)).astype(jnp.bfloat16))
        lane = lax.broadcasted_iota(jnp.int32, (count, LANES), 1)
        mine = lane % (LANES // 2) == ep
        weight = [
            jnp.sum(
                jnp.where(mine, gath[s, :, width:].astype(jnp.float32), 0.0), axis=1, keepdims=True
            )
            for s in slots
        ]
        step = width // 4
        for c in range(0, width, step):
            y = jnp.dot(acts[0], wd[0, :, c : c + step], preferred_element_type=jnp.float32)
            y = y + jnp.dot(acts[1], wd[1, :, c : c + step], preferred_element_type=jnp.float32)
            for i, s in enumerate(slots):
                contrib[s, :, c : c + step] = (
                    y[i * count : (i + 1) * count] * weight[i]
                ).astype(jnp.bfloat16)

    def back_x(slot, c):
        return pltpu.make_async_remote_copy(
            contrib.at[slot, pieces[c]], from_x.at[slot, pieces[c]],
            rx_send.at[slot, c], rx_recv.at[slot, c],
            device_id=x_peer, device_id_type=MESH,
        )

    def back_z(zz, slot, c):
        return pltpu.make_async_remote_copy(
            summed.at[zz, pieces[c]], from_z.at[slot, pieces[c]],
            rz_send.at[zz, c], rz_recv.at[slot, c],
            device_id=at_z(zz), device_id_type=MESH,
        )

    def final(c):
        part = res.at[pieces[c]]
        return pltpu.make_async_remote_copy(
            part, part, f_send.at[c], f_recv.at[c], device_id=sibling, device_id_type=MESH
        )

    def weights_here():
        for c in local:
            c.wait()
        for c in shared:
            c.wait()

    parts = range(len(pieces))
    cut = nz - 1
    early, late = order[:cut], order[cut:]
    back = early[1:][::-1] + late

    def pair_sum(slot, c):
        return contrib[slot, pieces[c]].astype(jnp.float32) + from_x[slot, pieces[c]].astype(
            jnp.float32
        )

    @pl.when(home)
    def _():
        for zz in others:
            for c in parts:
                along_z(zz, z, c).start()
        for c in parts:
            across_x(z, c).start()
        for slot in order[1:]:
            for c in parts:
                along_z(slot, slot, c).wait_recv()
                across_x(slot, c).start()
        weights_here()
        compute(order)
        for slot in back:
            for c in parts:
                back_x(slot, c).wait_recv()
                summed[slot, pieces[c]] = pair_sum(slot, c).astype(jnp.bfloat16)
                back_z(slot, z, c).start()
        for c in parts:
            back_x(z, c).wait_recv()
        for c in parts:
            total = pair_sum(z, c)
            for slot in order[1:]:
                back_z(slot, slot, c).wait_recv()
                total = total + from_z[slot, pieces[c]].astype(jnp.float32)
            res[pieces[c]] = total.astype(jnp.bfloat16)
            final(c).start()
            out_ref[pieces[c]] = total.astype(out_ref.dtype)
        for c in parts:
            for zz in others:
                along_z(zz, z, c).wait_send()
                back_z(zz, z, c).wait_send()
            for slot in order:
                across_x(slot, c).wait_send()
            final(c).wait_send()

    @pl.when(jnp.logical_not(home))
    def _():
        def take(slots):
            for slot in slots:
                for c in parts:
                    across_x(slot, c).wait_recv()

        def give(slots):
            for slot in slots:
                for c in parts:
                    back_x(slot, c).start()

        take(early)
        weights_here()
        compute(early)
        give(early[1:][::-1])
        take(late)
        compute(late)
        give(late)
        give(early[:1])
        for c in parts:
            for slot in order:
                back_x(slot, c).wait_send()
        for c in parts:
            final(c).wait_recv()
            out_ref[pieces[c]] = res[pieces[c]].astype(out_ref.dtype)


def gather_body(tokens, norm_gain, routes, gate_scores, w_gate, w_up, w_down):
    count, width = tokens.shape
    top = routes.shape[1]
    nz = lax.axis_size("ep") // 2
    hidden = w_gate.shape[2]
    bf16 = jnp.bfloat16
    dma = pltpu.SemaphoreType.DMA
    block = (nz, count, width)
    vmem = pl.BlockSpec(memory_space=pltpu.VMEM)
    hbm = pl.BlockSpec(memory_space=pltpu.HBM)
    out = pl.pallas_call(
        functools.partial(moe_kernel, nz),
        out_shape=pltpu.VMEM((count, width), bf16),
        in_specs=[hbm] * 7,
        out_specs=vmem,
        scratch_shapes=[
            pltpu.VMEM((count, width), bf16),
            pltpu.VMEM((1, width), jnp.float32),
            pltpu.VMEM((top, count), jnp.int32),
            pltpu.VMEM((top, count), jnp.float32),
            pltpu.VMEM((nz, count, width + LANES), bf16),
            pltpu.VMEM((2, width, hidden), bf16),
            pltpu.VMEM((2, width, hidden), bf16),
            pltpu.VMEM((2, hidden, width), bf16),
            pltpu.VMEM(block, bf16),
            pltpu.VMEM(block, bf16),
            pltpu.VMEM(block, bf16),
            pltpu.VMEM(block, bf16),
            pltpu.VMEM((count, width), bf16),
        ]
        + [dma((4,))]
        + [dma((3,))] * 3
        + [dma((nz, count // ROWS))] * 8
        + [dma((count // ROWS,))] * 2,
        compiler_params=pltpu.CompilerParams(
            collective_id=0, has_side_effects=True, vmem_limit_bytes=VMEM_BYTES
        ),
        name="moe",
    )(tokens, norm_gain.reshape(1, width), routes.T, gate_scores.T, w_gate, w_up, w_down)
    return out


def body(tokens, norm_gain, routes, gate_scores, w_gate, w_up, w_down):
    nexp = lax.axis_size("ep")
    every_row = 2 * routes.shape[1] >= nexp
    pairs = lax.axis_size("tp") == 2 and nexp % 2 == 0
    one = exchange_body
    whole_rows = tokens.shape[0] % ROWS == 0
    if whole_rows and every_row and pairs and w_gate.shape[0] == 1 and 2 * nexp <= LANES:
        one = gather_body
    return one(tokens, norm_gain, routes, gate_scores, w_gate, w_up, w_down)


def solution(mesh):
    in_specs = (
        P(("grp", "ep"), None),
        P(),
        P(("grp", "ep"), None),
        P(("grp", "ep"), None),
        P("ep", None, "tp"),
        P("ep", None, "tp"),
        P("ep", "tp", None),
    )
    out_specs = P(("grp", "ep"), None)
    return jax.shard_map(body, mesh=mesh, in_specs=in_specs, out_specs=out_specs, check_vma=False)
```

```python
import functools

import jax
import jax.numpy as jnp
from jax import lax
from jax.experimental import pallas as pl
from jax.experimental.pallas import tpu as pltpu
from jax.sharding import PartitionSpec as P

MESH = pl.DeviceIdType.MESH
LANES = 128


def clamped_unit(g, u):
    gate = jnp.minimum(g, 7.0)
    up = jnp.clip(u, -7.0, 7.0)
    return (up + 1.0) * gate * jax.nn.sigmoid(1.702 * gate)


def expert_rows(rows, wg, wu, wd):
    g = jnp.dot(rows, wg, preferred_element_type=jnp.float32)
    u = jnp.dot(rows, wu, preferred_element_type=jnp.float32)
    act = clamped_unit(g, u).astype(jnp.bfloat16)
    part = jnp.dot(act, wd, preferred_element_type=jnp.float32)
    part = lax.optimization_barrier(part.astype(jnp.bfloat16)).astype(jnp.float32)
    total = lax.psum(part.astype(jnp.bfloat16), "tp")
    return total


def finish(mixed):
    result = mixed.astype(jnp.bfloat16)
    return result


def slot_table(routes, scores, experts, capacity):
    count = routes.shape[0]
    chosen = routes[:, :, None] == experts[None, None, :]
    hit = jnp.any(chosen, axis=1).astype(jnp.int32)
    weight = jnp.sum(jnp.where(chosen, scores[:, :, None], 0.0), axis=1)
    rank = jnp.cumsum(hit, axis=0) - hit
    places = jnp.arange(capacity, dtype=jnp.int32)
    match = (hit[:, :, None] == 1) & (rank[:, :, None] == places[None, None, :])
    row_ids = jnp.arange(count, dtype=jnp.int32)[:, None, None]
    filled = jnp.any(match, axis=0)
    slot_tok = jnp.sum(jnp.where(match, row_ids, 0), axis=0) + count * (
        1 - filled.astype(jnp.int32)
    )
    slot_w = jnp.sum(jnp.where(match, weight[:, :, None], 0.0), axis=0)
    return (slot_tok, slot_w)


def exchange_body(tokens, norm_gain, routes, gate_scores, w_gate, w_up, w_down):
    count, width = tokens.shape
    top = routes.shape[1]
    nexp = lax.axis_size("ep")
    capacity = max(2, min(count, 2 * count * top // nexp))
    wg, wu, wd = (w_gate[0], w_up[0], w_down[0])
    xf = tokens.astype(jnp.float32)
    normed = (xf * lax.rsqrt(jnp.mean(xf * xf, axis=-1, keepdims=True) + 1e-06) * norm_gain).astype(
        jnp.bfloat16
    )
    experts = jnp.arange(nexp, dtype=jnp.int32)
    slot_tok, slot_w = slot_table(routes, gate_scores, experts, capacity)
    padded = jnp.concatenate([normed, jnp.zeros((1, width), jnp.bfloat16)], axis=0)
    outgoing = padded[slot_tok]
    received = lax.all_to_all(outgoing, "ep", split_axis=0, concat_axis=0, tiled=True)
    sources, places, _ = received.shape
    outputs = expert_rows(received.reshape(sources * places, width), wg, wu, wd)
    returned = lax.all_to_all(
        outputs.reshape(sources, places, outputs.shape[1]),
        "ep",
        split_axis=0,
        concat_axis=0,
        tiled=True,
    )
    flat_tok = slot_tok.reshape(-1)
    token_ids = jnp.arange(count, dtype=jnp.int32)
    combine = jnp.where(flat_tok[None, :] == token_ids[:, None], slot_w.reshape(-1)[None, :], 0.0)
    mixed = jnp.dot(
        combine,
        returned.reshape(-1, returned.shape[2]).astype(jnp.float32),
        precision=lax.Precision.HIGHEST,
    )
    return finish(mixed)


VMEM_BYTES = 66500000
ROWS = 8


def moe_kernel(
    nz,
    tok_hbm, gain_hbm, routes_hbm, score_hbm, wg_hbm, wu_hbm, wd_hbm,
    out_ref,
    tok_ref, gain_ref, routes_ref, score_ref, gath, wg, wu, wd, contrib, from_x, summed, from_z, from_far, res,
    in_sem, w_loc, w_send, w_recv, z_send, z_recv, x_send, x_recv,
    rx_send, rx_recv, rz_send, rz_recv, far_send, far_recv, f_send, f_recv,
):
    ep, tp = lax.axis_index("ep"), lax.axis_index("tp")
    z, x = ep // 2, ep % 2
    home = x == tp
    count, width = tok_hbm.shape

    def at_z(zz):
        return {"ep": zz * 2 + x, "tp": tp}

    x_peer = {"ep": z * 2 + 1 - x, "tp": tp}
    sibling = {"ep": ep, "tp": 1 - tp}
    opposite = (z + nz // 2) % nz
    others = [(z + k) % nz for k in range(1, nz) if k != nz // 2] + [opposite]
    order = [z] + others
    x_opposite = {"ep": opposite * 2 + 1 - x, "tp": tp}
    pieces = [pl.ds(r, ROWS) for r in range(0, count, ROWS)]

    barrier = pltpu.get_barrier_semaphore()
    for zz in others:
        pl.semaphore_signal(barrier, inc=1, device_id=at_z(zz), device_id_type=MESH)
    pl.semaphore_signal(barrier, inc=1, device_id=x_peer, device_id_type=MESH)
    pl.semaphore_signal(barrier, inc=1, device_id=x_opposite, device_id_type=MESH)
    pl.semaphore_signal(barrier, inc=1, device_id=sibling, device_id_type=MESH)

    weights = ((wg_hbm, wg), (wu_hbm, wu), (wd_hbm, wd))
    local = [
        pltpu.make_async_copy(src.at[0], dst.at[tp], w_loc.at[i])
        for i, (src, dst) in enumerate(weights)
    ]
    shared = [
        pltpu.make_async_remote_copy(
            src.at[0], dst.at[tp], w_send.at[i], w_recv.at[i], device_id=sibling, device_id_type=MESH
        )
        for i, (src, dst) in enumerate(weights)
    ]
    inputs = [
        pltpu.make_async_copy(src, dst, in_sem.at[i])
        for i, (src, dst) in enumerate(
            ((tok_hbm, tok_ref), (gain_hbm, gain_ref), (routes_hbm, routes_ref), (score_hbm, score_ref))
        )
    ]
    for c in local:
        c.start()

    @pl.when(home)
    def _():
        for c in inputs:
            c.start()
        for c in inputs:
            c.wait()
        xf = tok_ref[...].astype(jnp.float32)
        scale = lax.rsqrt(jnp.mean(xf * xf, axis=-1, keepdims=True) + 1e-06)
        gath[z, :, :width] = (xf * scale * gain_ref[...]).astype(jnp.bfloat16)
        line = lax.broadcasted_iota(jnp.int32, (LANES, count), 0)
        half = LANES // 2
        expert = line % half
        w = jnp.zeros((LANES, count), jnp.float32)
        for k in range(routes_ref.shape[0]):
            w = w + jnp.where(routes_ref[k : k + 1, :] == expert, score_ref[k : k + 1, :], 0.0)
        high = w.astype(jnp.bfloat16).astype(jnp.float32)
        gath[z, :, width:] = jnp.where(line < half, high, w - high).T.astype(jnp.bfloat16)

    pl.semaphore_wait(barrier, nz + 2)
    for c in shared:
        c.start()

    def along_z(zz, slot, c):
        part = gath.at[slot, pieces[c]]
        return pltpu.make_async_remote_copy(
            part, part, z_send.at[zz, c], z_recv.at[slot, c],
            device_id=at_z(zz), device_id_type=MESH,
        )

    def across_x(slot, c):
        part = gath.at[slot, pieces[c]]
        return pltpu.make_async_remote_copy(
            part, part, x_send.at[slot, c], x_recv.at[slot, c],
            device_id=x_peer, device_id_type=MESH,
        )

    def compute(slots):
        rows = jnp.concatenate(
            [gath[s, :, :width].astype(jnp.float32) for s in slots], axis=0
        ).astype(jnp.bfloat16)
        acts = []
        for j in range(2):
            g = jnp.dot(rows, wg[j], preferred_element_type=jnp.float32)
            u = jnp.dot(rows, wu[j], preferred_element_type=jnp.float32)
            gate = jnp.minimum(g, 7.0)
            up = jnp.clip(u, -7.0, 7.0)
            acts.append(((up + 1.0) * gate * jax.nn.sigmoid(1.702 * gate)).astype(jnp.bfloat16))
        lane = lax.broadcasted_iota(jnp.int32, (count, LANES), 1)
        mine = lane % (LANES // 2) == ep
        weight = [
            jnp.sum(
                jnp.where(mine, gath[s, :, width:].astype(jnp.float32), 0.0), axis=1, keepdims=True
            )
            for s in slots
        ]
        step = width // 4
        for c in range(0, width, step):
            y = jnp.dot(acts[0], wd[0, :, c : c + step], preferred_element_type=jnp.float32)
            y = y + jnp.dot(acts[1], wd[1, :, c : c + step], preferred_element_type=jnp.float32)
            for i, s in enumerate(slots):
                contrib[s, :, c : c + step] = (
                    y[i * count : (i + 1) * count] * weight[i]
                ).astype(jnp.bfloat16)

    def back_x(slot, c):
        return pltpu.make_async_remote_copy(
            contrib.at[slot, pieces[c]], from_x.at[slot, pieces[c]],
            rx_send.at[slot, c], rx_recv.at[slot, c],
            device_id=x_peer, device_id_type=MESH,
        )

    def straight(slot, c):
        return pltpu.make_async_remote_copy(
            contrib.at[slot, pieces[c]], from_far.at[pieces[c]], far_send.at[c], far_recv.at[c],
            device_id=x_opposite, device_id_type=MESH,
        )

    def back_z(zz, slot, c, source=summed):
        return pltpu.make_async_remote_copy(
            source.at[zz, pieces[c]], from_z.at[slot, pieces[c]],
            rz_send.at[zz, c], rz_recv.at[slot, c],
            device_id=at_z(zz), device_id_type=MESH,
        )

    def final(c):
        part = res.at[pieces[c]]
        return pltpu.make_async_remote_copy(
            part, part, f_send.at[c], f_recv.at[c], device_id=sibling, device_id_type=MESH
        )

    def weights_here():
        for c in local:
            c.wait()
        for c in shared:
            c.wait()

    parts = range(len(pieces))
    early = order[:-1]

    def pair_sum(slot, c):
        return contrib[slot, pieces[c]].astype(jnp.float32) + from_x[slot, pieces[c]].astype(
            jnp.float32
        )

    @pl.when(home)
    def _():
        for zz in others:
            for c in parts:
                along_z(zz, z, c).start()
        for c in parts:
            across_x(z, c).start()
        for slot in order[1:]:
            for c in parts:
                along_z(slot, slot, c).wait_recv()
                across_x(slot, c).start()
        weights_here()
        compute(order)
        for c in parts:
            back_z(opposite, z, c, contrib).start()
        for slot in early[1:]:
            for c in parts:
                back_x(slot, c).wait_recv()
                summed[slot, pieces[c]] = pair_sum(slot, c).astype(jnp.bfloat16)
                back_z(slot, z, c).start()
        for c in parts:
            back_x(z, c).wait_recv()
        for c in parts:
            total = pair_sum(z, c)
            straight(z, c).wait_recv()
            total = total + from_far[pieces[c]].astype(jnp.float32)
            for slot in order[1:]:
                back_z(slot, slot, c).wait_recv()
                total = total + from_z[slot, pieces[c]].astype(jnp.float32)
            res[pieces[c]] = total.astype(jnp.bfloat16)
            final(c).start()
            out_ref[pieces[c]] = total.astype(out_ref.dtype)
        for c in parts:
            for zz in others:
                along_z(zz, z, c).wait_send()
                back_z(zz, z, c).wait_send()
            for slot in order:
                across_x(slot, c).wait_send()
            final(c).wait_send()

    @pl.when(jnp.logical_not(home))
    def _():
        def take(slots):
            for slot in slots:
                for c in parts:
                    across_x(slot, c).wait_recv()

        def give(slots):
            for slot in slots:
                for c in parts:
                    back_x(slot, c).start()

        done = 0
        for size in (nz - 2, 1, 1):
            slots = order[done : done + size]
            done += size
            take(slots)
            if size == done:
                weights_here()
            compute(slots)
            if slots[-1] is opposite:
                for c in parts:
                    straight(opposite, c).start()
            give([s for s in slots if s is not z and s is not opposite])
        give([z])
        for c in parts:
            straight(opposite, c).wait_send()
        for c in parts:
            for slot in early:
                back_x(slot, c).wait_send()
        for c in parts:
            final(c).wait_recv()
            out_ref[pieces[c]] = res[pieces[c]].astype(out_ref.dtype)


def gather_body(tokens, norm_gain, routes, gate_scores, w_gate, w_up, w_down):
    count, width = tokens.shape
    top = routes.shape[1]
    nz = lax.axis_size("ep") // 2
    hidden = w_gate.shape[2]
    bf16 = jnp.bfloat16
    dma = pltpu.SemaphoreType.DMA
    block = (nz, count, width)
    vmem = pl.BlockSpec(memory_space=pltpu.VMEM)
    hbm = pl.BlockSpec(memory_space=pltpu.HBM)
    out = pl.pallas_call(
        functools.partial(moe_kernel, nz),
        out_shape=pltpu.VMEM((count, width), bf16),
        in_specs=[hbm] * 7,
        out_specs=vmem,
        scratch_shapes=[
            pltpu.VMEM((count, width), bf16),
            pltpu.VMEM((1, width), jnp.float32),
            pltpu.VMEM((top, count), jnp.int32),
            pltpu.VMEM((top, count), jnp.float32),
            pltpu.VMEM((nz, count, width + LANES), bf16),
            pltpu.VMEM((2, width, hidden), bf16),
            pltpu.VMEM((2, width, hidden), bf16),
            pltpu.VMEM((2, hidden, width), bf16),
            pltpu.VMEM(block, bf16),
            pltpu.VMEM(block, bf16),
            pltpu.VMEM(block, bf16),
            pltpu.VMEM(block, bf16),
            pltpu.VMEM((count, width), bf16),
            pltpu.VMEM((count, width), bf16),
        ]
        + [dma((4,))]
        + [dma((3,))] * 3
        + [dma((nz, count // ROWS))] * 8
        + [dma((count // ROWS,))] * 4,
        compiler_params=pltpu.CompilerParams(
            collective_id=0, has_side_effects=True, vmem_limit_bytes=VMEM_BYTES
        ),
        name="moe",
    )(tokens, norm_gain.reshape(1, width), routes.T, gate_scores.T, w_gate, w_up, w_down)
    return out


def body(tokens, norm_gain, routes, gate_scores, w_gate, w_up, w_down):
    nexp = lax.axis_size("ep")
    every_row = 2 * routes.shape[1] >= nexp
    pairs = lax.axis_size("tp") == 2 and nexp % 4 == 0 and nexp >= 8
    one = exchange_body
    whole_rows = tokens.shape[0] % ROWS == 0
    if whole_rows and every_row and pairs and w_gate.shape[0] == 1 and 2 * nexp <= LANES:
        one = gather_body
    return one(tokens, norm_gain, routes, gate_scores, w_gate, w_up, w_down)


def solution(mesh):
    in_specs = (
        P(("grp", "ep"), None),
        P(),
        P(("grp", "ep"), None),
        P(("grp", "ep"), None),
        P("ep", None, "tp"),
        P("ep", None, "tp"),
        P("ep", "tp", None),
    )
    out_specs = P(("grp", "ep"), None)
    return jax.shard_map(body, mesh=mesh, in_specs=in_specs, out_specs=out_specs, check_vma=False)
```

```python
import functools

import jax
import jax.numpy as jnp
from jax import lax
from jax.experimental import pallas as pl
from jax.experimental.pallas import tpu as pltpu
from jax.sharding import PartitionSpec as P

MESH = pl.DeviceIdType.MESH
LANES = 128


def clamped_unit(g, u):
    gate = jnp.minimum(g, 7.0)
    up = jnp.clip(u, -7.0, 7.0)
    return (up + 1.0) * gate * jax.nn.sigmoid(1.702 * gate)


def expert_rows(rows, wg, wu, wd):
    g = jnp.dot(rows, wg, preferred_element_type=jnp.float32)
    u = jnp.dot(rows, wu, preferred_element_type=jnp.float32)
    act = clamped_unit(g, u).astype(jnp.bfloat16)
    part = jnp.dot(act, wd, preferred_element_type=jnp.float32)
    part = lax.optimization_barrier(part.astype(jnp.bfloat16)).astype(jnp.float32)
    total = lax.psum(part.astype(jnp.bfloat16), "tp")
    return total


def finish(mixed):
    result = mixed.astype(jnp.bfloat16)
    return result


def slot_table(routes, scores, experts, capacity):
    count = routes.shape[0]
    chosen = routes[:, :, None] == experts[None, None, :]
    hit = jnp.any(chosen, axis=1).astype(jnp.int32)
    weight = jnp.sum(jnp.where(chosen, scores[:, :, None], 0.0), axis=1)
    rank = jnp.cumsum(hit, axis=0) - hit
    places = jnp.arange(capacity, dtype=jnp.int32)
    match = (hit[:, :, None] == 1) & (rank[:, :, None] == places[None, None, :])
    row_ids = jnp.arange(count, dtype=jnp.int32)[:, None, None]
    filled = jnp.any(match, axis=0)
    slot_tok = jnp.sum(jnp.where(match, row_ids, 0), axis=0) + count * (
        1 - filled.astype(jnp.int32)
    )
    slot_w = jnp.sum(jnp.where(match, weight[:, :, None], 0.0), axis=0)
    return (slot_tok, slot_w)


def exchange_body(tokens, norm_gain, routes, gate_scores, w_gate, w_up, w_down):
    count, width = tokens.shape
    top = routes.shape[1]
    nexp = lax.axis_size("ep")
    capacity = max(2, min(count, 2 * count * top // nexp))
    wg, wu, wd = (w_gate[0], w_up[0], w_down[0])
    xf = tokens.astype(jnp.float32)
    normed = (xf * lax.rsqrt(jnp.mean(xf * xf, axis=-1, keepdims=True) + 1e-06) * norm_gain).astype(
        jnp.bfloat16
    )
    experts = jnp.arange(nexp, dtype=jnp.int32)
    slot_tok, slot_w = slot_table(routes, gate_scores, experts, capacity)
    padded = jnp.concatenate([normed, jnp.zeros((1, width), jnp.bfloat16)], axis=0)
    outgoing = padded[slot_tok]
    received = lax.all_to_all(outgoing, "ep", split_axis=0, concat_axis=0, tiled=True)
    sources, places, _ = received.shape
    outputs = expert_rows(received.reshape(sources * places, width), wg, wu, wd)
    returned = lax.all_to_all(
        outputs.reshape(sources, places, outputs.shape[1]),
        "ep",
        split_axis=0,
        concat_axis=0,
        tiled=True,
    )
    flat_tok = slot_tok.reshape(-1)
    token_ids = jnp.arange(count, dtype=jnp.int32)
    combine = jnp.where(flat_tok[None, :] == token_ids[:, None], slot_w.reshape(-1)[None, :], 0.0)
    mixed = jnp.dot(
        combine,
        returned.reshape(-1, returned.shape[2]).astype(jnp.float32),
        precision=lax.Precision.HIGHEST,
    )
    return finish(mixed)


VMEM_BYTES = 66500000
ROWS = 8


def moe_kernel(
    nz,
    tok_hbm, gain_hbm, routes_hbm, score_hbm, wg_hbm, wu_hbm, wd_hbm,
    out_ref,
    tok_ref, gain_ref, routes_ref, score_ref, gath, wg, wu, wd, contrib, from_x, summed, from_z, from_far, res,
    in_sem, w_loc, w_send, w_recv, z_send, z_recv, x_send, x_recv,
    rx_send, rx_recv, rz_send, rz_recv, far_send, far_recv, f_send, f_recv,
):
    ep, tp = lax.axis_index("ep"), lax.axis_index("tp")
    z, x = ep // 2, ep % 2
    home = x == tp
    count, width = tok_hbm.shape

    def at_z(zz):
        return {"ep": zz * 2 + x, "tp": tp}

    x_peer = {"ep": z * 2 + 1 - x, "tp": tp}
    sibling = {"ep": ep, "tp": 1 - tp}
    opposite = (z + nz // 2) % nz
    others = [(z + k) % nz for k in range(1, nz) if k != nz // 2] + [opposite]
    order = [z] + others
    x_opposite = {"ep": opposite * 2 + 1 - x, "tp": tp}
    pieces = [pl.ds(r, ROWS) for r in range(0, count, ROWS)]

    barrier = pltpu.get_barrier_semaphore()
    for zz in others:
        pl.semaphore_signal(barrier, inc=1, device_id=at_z(zz), device_id_type=MESH)
    pl.semaphore_signal(barrier, inc=1, device_id=x_peer, device_id_type=MESH)
    pl.semaphore_signal(barrier, inc=1, device_id=x_opposite, device_id_type=MESH)
    pl.semaphore_signal(barrier, inc=1, device_id=sibling, device_id_type=MESH)

    weights = ((wg_hbm, wg), (wu_hbm, wu), (wd_hbm, wd))
    local = [
        pltpu.make_async_copy(src.at[0], dst.at[tp], w_loc.at[i])
        for i, (src, dst) in enumerate(weights)
    ]
    shared = [
        pltpu.make_async_remote_copy(
            src.at[0], dst.at[tp], w_send.at[i], w_recv.at[i], device_id=sibling, device_id_type=MESH
        )
        for i, (src, dst) in enumerate(weights)
    ]
    inputs = [
        pltpu.make_async_copy(src, dst, in_sem.at[i])
        for i, (src, dst) in enumerate(
            ((tok_hbm, tok_ref), (gain_hbm, gain_ref), (routes_hbm, routes_ref), (score_hbm, score_ref))
        )
    ]
    for c in local:
        c.start()

    @pl.when(home)
    def _():
        for c in inputs:
            c.start()
        for c in inputs:
            c.wait()
        xf = tok_ref[...].astype(jnp.float32)
        scale = lax.rsqrt(jnp.mean(xf * xf, axis=-1, keepdims=True) + 1e-06)
        gath[z, :, :width] = (xf * scale * gain_ref[...]).astype(jnp.bfloat16)
        line = lax.broadcasted_iota(jnp.int32, (LANES, count), 0)
        half = LANES // 2
        expert = line % half
        w = jnp.zeros((LANES, count), jnp.float32)
        for k in range(routes_ref.shape[0]):
            w = w + jnp.where(routes_ref[k : k + 1, :] == expert, score_ref[k : k + 1, :], 0.0)
        high = w.astype(jnp.bfloat16).astype(jnp.float32)
        gath[z, :, width:] = jnp.where(line < half, high, w - high).T.astype(jnp.bfloat16)

    pl.semaphore_wait(barrier, nz + 2)
    for c in shared:
        c.start()

    def along_z(zz, slot, c):
        part = gath.at[slot, pieces[c]]
        return pltpu.make_async_remote_copy(
            part, part, z_send.at[zz, c], z_recv.at[slot, c],
            device_id=at_z(zz), device_id_type=MESH,
        )

    def across_x(slot, c):
        part = gath.at[slot, pieces[c]]
        return pltpu.make_async_remote_copy(
            part, part, x_send.at[slot, c], x_recv.at[slot, c],
            device_id=x_peer, device_id_type=MESH,
        )

    def compute(slots):
        rows = jnp.concatenate(
            [gath[s, :, :width].astype(jnp.float32) for s in slots], axis=0
        ).astype(jnp.bfloat16)
        acts = []
        for j in range(2):
            g = jnp.dot(rows, wg[j], preferred_element_type=jnp.float32)
            u = jnp.dot(rows, wu[j], preferred_element_type=jnp.float32)
            gate = jnp.minimum(g, 7.0)
            up = jnp.clip(u, -7.0, 7.0)
            acts.append(((up + 1.0) * gate * jax.nn.sigmoid(1.702 * gate)).astype(jnp.bfloat16))
        lane = lax.broadcasted_iota(jnp.int32, (count, LANES), 1)
        mine = lane % (LANES // 2) == ep
        weight = [
            jnp.sum(
                jnp.where(mine, gath[s, :, width:].astype(jnp.float32), 0.0), axis=1, keepdims=True
            )
            for s in slots
        ]
        step = width // 4
        for c in range(0, width, step):
            y = jnp.dot(acts[0], wd[0, :, c : c + step], preferred_element_type=jnp.float32)
            y = y + jnp.dot(acts[1], wd[1, :, c : c + step], preferred_element_type=jnp.float32)
            for i, s in enumerate(slots):
                contrib[s, :, c : c + step] = (
                    y[i * count : (i + 1) * count] * weight[i]
                ).astype(jnp.bfloat16)

    def back_x(slot, c):
        return pltpu.make_async_remote_copy(
            contrib.at[slot, pieces[c]], from_x.at[slot, pieces[c]],
            rx_send.at[slot, c], rx_recv.at[slot, c],
            device_id=x_peer, device_id_type=MESH,
        )

    def straight(slot, c):
        return pltpu.make_async_remote_copy(
            contrib.at[slot, pieces[c]], from_far.at[pieces[c]], far_send.at[c], far_recv.at[c],
            device_id=x_opposite, device_id_type=MESH,
        )

    def back_z(zz, slot, c, source=summed):
        return pltpu.make_async_remote_copy(
            source.at[zz, pieces[c]], from_z.at[slot, pieces[c]],
            rz_send.at[zz, c], rz_recv.at[slot, c],
            device_id=at_z(zz), device_id_type=MESH,
        )

    def final(c):
        part = res.at[pieces[c]]
        return pltpu.make_async_remote_copy(
            part, part, f_send.at[c], f_recv.at[c], device_id=sibling, device_id_type=MESH
        )

    def weights_here():
        for c in local:
            c.wait()
        for c in shared:
            c.wait()

    parts = range(len(pieces))
    early = order[:-1]

    def pair_sum(slot, c):
        return contrib[slot, pieces[c]].astype(jnp.float32) + from_x[slot, pieces[c]].astype(
            jnp.float32
        )

    @pl.when(home)
    def _():
        for zz in others:
            for c in parts:
                along_z(zz, z, c).start()
        for c in parts:
            across_x(z, c).start()
        for slot in order[1:]:
            for c in parts:
                along_z(slot, slot, c).wait_recv()
                across_x(slot, c).start()
        weights_here()
        compute(order)
        for c in parts:
            back_z(opposite, z, c, contrib).start()
        for slot in early[1:]:
            for c in parts:
                back_x(slot, c).wait_recv()
                summed[slot, pieces[c]] = pair_sum(slot, c).astype(jnp.bfloat16)
                back_z(slot, z, c).start()
        for c in parts:
            back_x(z, c).wait_recv()
        for c in parts:
            total = pair_sum(z, c)
            straight(z, c).wait_recv()
            total = total + from_far[pieces[c]].astype(jnp.float32)
            for slot in order[1:]:
                back_z(slot, slot, c).wait_recv()
                total = total + from_z[slot, pieces[c]].astype(jnp.float32)
            res[pieces[c]] = total.astype(jnp.bfloat16)
            final(c).start()
            out_ref[pieces[c]] = total.astype(out_ref.dtype)
        for c in parts:
            for zz in others:
                along_z(zz, z, c).wait_send()
                back_z(zz, z, c).wait_send()
            for slot in order:
                across_x(slot, c).wait_send()
            final(c).wait_send()

    @pl.when(jnp.logical_not(home))
    def _():
        def take(slots):
            for slot in slots:
                for c in parts:
                    across_x(slot, c).wait_recv()

        def give(slots):
            for slot in slots:
                for c in parts:
                    back_x(slot, c).start()

        done = 0
        for size in (nz - 2, 1, 1):
            slots = order[done : done + size]
            done += size
            take(slots)
            if size == done:
                weights_here()
            compute(slots)
            if slots[-1] is opposite:
                for c in parts:
                    straight(opposite, c).start()
            give([s for s in slots if s is not z and s is not opposite])
            if done == nz - 1:
                give([z])
        for c in parts:
            straight(opposite, c).wait_send()
        for c in parts:
            for slot in early:
                back_x(slot, c).wait_send()
        for c in parts:
            final(c).wait_recv()
            out_ref[pieces[c]] = res[pieces[c]].astype(out_ref.dtype)


def gather_body(tokens, norm_gain, routes, gate_scores, w_gate, w_up, w_down):
    count, width = tokens.shape
    top = routes.shape[1]
    nz = lax.axis_size("ep") // 2
    hidden = w_gate.shape[2]
    bf16 = jnp.bfloat16
    dma = pltpu.SemaphoreType.DMA
    block = (nz, count, width)
    vmem = pl.BlockSpec(memory_space=pltpu.VMEM)
    hbm = pl.BlockSpec(memory_space=pltpu.HBM)
    out = pl.pallas_call(
        functools.partial(moe_kernel, nz),
        out_shape=pltpu.VMEM((count, width), bf16),
        in_specs=[hbm] * 7,
        out_specs=vmem,
        scratch_shapes=[
            pltpu.VMEM((count, width), bf16),
            pltpu.VMEM((1, width), jnp.float32),
            pltpu.VMEM((top, count), jnp.int32),
            pltpu.VMEM((top, count), jnp.float32),
            pltpu.VMEM((nz, count, width + LANES), bf16),
            pltpu.VMEM((2, width, hidden), bf16),
            pltpu.VMEM((2, width, hidden), bf16),
            pltpu.VMEM((2, hidden, width), bf16),
            pltpu.VMEM(block, bf16),
            pltpu.VMEM(block, bf16),
            pltpu.VMEM(block, bf16),
            pltpu.VMEM(block, bf16),
            pltpu.VMEM((count, width), bf16),
            pltpu.VMEM((count, width), bf16),
        ]
        + [dma((4,))]
        + [dma((3,))] * 3
        + [dma((nz, count // ROWS))] * 8
        + [dma((count // ROWS,))] * 4,
        compiler_params=pltpu.CompilerParams(
            collective_id=0, has_side_effects=True, vmem_limit_bytes=VMEM_BYTES
        ),
        name="moe",
    )(tokens, norm_gain.reshape(1, width), routes.T, gate_scores.T, w_gate, w_up, w_down)
    return out


def body(tokens, norm_gain, routes, gate_scores, w_gate, w_up, w_down):
    nexp = lax.axis_size("ep")
    every_row = 2 * routes.shape[1] >= nexp
    pairs = lax.axis_size("tp") == 2 and nexp % 4 == 0 and nexp >= 8
    one = exchange_body
    whole_rows = tokens.shape[0] % ROWS == 0
    if whole_rows and every_row and pairs and w_gate.shape[0] == 1 and 2 * nexp <= LANES:
        one = gather_body
    return one(tokens, norm_gain, routes, gate_scores, w_gate, w_up, w_down)


def solution(mesh):
    in_specs = (
        P(("grp", "ep"), None),
        P(),
        P(("grp", "ep"), None),
        P(("grp", "ep"), None),
        P("ep", None, "tp"),
        P("ep", None, "tp"),
        P("ep", "tp", None),
    )
    out_specs = P(("grp", "ep"), None)
    return jax.shard_map(body, mesh=mesh, in_specs=in_specs, out_specs=out_specs, check_vma=False)
```
